32 devices in a mesh: ep: 16 (over z, y, x), tp: 2 (over core).
Axes of the slice: x: 2, y: 2, z: 4, core: 2. Of those that a mesh axis runs over, the one named last changes fastest.
Arguments:
- tokens: bfloat16 [512, 1024], P(('ep', 'tp')), may hold values from -6 to 6
- lengths: int32 [512], P(('ep', 'tp')), may hold values from 1 to 1024
- cache_latent: bfloat16 [512, 1024, 256], P(('ep', 'tp')), may hold values from -700 to 700
- cache_rope: bfloat16 [512, 32, 1024], P(('ep', 'tp')), may hold values from -6 to 6
- attn_gain: bfloat16 [1024], replicated, may hold values from 0.099609375 to 1.8984375
- w_dq: bfloat16 [1024, 512], replicated, may hold values from -0.1875 to 0.1875
- q_gain: bfloat16 [512], replicated, may hold values from 0.099609375 to 1.8984375
- w_q_nope: bfloat16 [512, 1024], replicated, may hold values from -0.25 to 0.25
- w_q_rope: bfloat16 [512, 512], replicated, may hold values from -0.25 to 0.25
- w_dkv: bfloat16 [1024, 256], replicated, may hold values from -0.1875 to 0.1875
- kv_gain: bfloat16 [256], replicated, may hold values from 0.099609375 to 1.8984375
- w_krope: bfloat16 [1024, 32], replicated, may hold values from -0.1875 to 0.1875
- w_uk: bfloat16 [256, 1024], replicated, may hold values from -0.75 to 0.75
- w_uv: bfloat16 [256, 1024], replicated, may hold values from -0.375 to 0.375
- w_o: bfloat16 [1024, 1024], replicated, may hold values from -0.1875 to 0.1875
- post_gain: bfloat16 [1024], replicated, may hold values from 0.099609375 to 1.8984375
- moe_gain: bfloat16 [1024], replicated, may hold values from 0.099609375 to 1.8984375
- routes: int32 [512, 4], P(('ep', 'tp')), may hold values from 0 to 15, all different within a row; in each aligned block of 16 rows (0 to 15, 16 to 31, ...) at most 6 rows name the same one
- route_scores: float32 [512, 4], P(('ep', 'tp')), may hold values from 0.05 to 1
- expert_gate: bfloat16 [16, 1024, 512], P('ep', None, 'tp'), may hold values from -0.1875 to 0.1875
- expert_up: bfloat16 [16, 1024, 512], P('ep', None, 'tp'), may hold values from -0.1875 to 0.1875
- expert_down: bfloat16 [16, 512, 1024], P('ep', 'tp'), may hold values from -0.25 to 0.25
- shared_gate: bfloat16 [1024, 512], replicated, may hold values from -0.1875 to 0.1875
- shared_up: bfloat16 [1024, 512], replicated, may hold values from -0.1875 to 0.1875
- shared_down: bfloat16 [512, 1024], replicated, may hold values from -0.25 to 0.25
- dense_vec: bfloat16 [1024], replicated, may hold values from -0.1875 to 0.1875
- dense_w_gate: bfloat16 [1024, 8192], P(None, ('ep', 'tp')), may hold values from -0.1875 to 0.1875
- dense_w_up: bfloat16 [1024, 8192], P(None, ('ep', 'tp')), may hold values from -0.1875 to 0.1875
- dense_w_down: bfloat16 [8192, 1024], P(('ep', 'tp')), may hold values from -0.125 to 0.125
- out_gain: bfloat16 [1024], replicated, may hold values from 0.099609375 to 1.8984375
Outputs:
- hidden_out: bfloat16 [512, 1024], P(('ep', 'tp'))
- new_latent: bfloat16 [512, 256], P(('ep', 'tp'))
The draws below stay inside these ranges and needn't reach their ends.
Inputs may be any that keep to these rules, and one draw needn't show every extreme that they name: `routes`: each row names 4 different experts. In the 16 rows of one device no expert is named more than 6 times, a bound that some block reaches in some devices' rows.
All inputs are finite; a program needn't handle non-finite values.
Results may differ from the reference program's by a relative error of at most 0.011.
The reference program's roundings to bfloat16 on the way count: a program that leaves them out, or rounds other values in their place, can miss the bound.
Values may be sent and summed in bfloat16 or wider, within the bound.
A program may use at most 128 MiB of HBM per device.

```python
import math
from functools import partial
import jax
import jax.numpy as jnp
import numpy as np
from jax import lax

D = 1024
HEADS = 16
QL = 512
KL = 256
NOPE = 64
ROPE = 32
VDIM = 64
EFF = 512
SFF = 512
DFF = 8192
TOP_K = 4
SEQ_DEV = 16
CACHE_LEN = 1024
EXPERTS = 16
CAP = 6
TOKENS = 512
N_TP = 2


def draw_cache_latent(key, part):
    base = jnp.clip(jax.random.normal(key, (TOKENS, CACHE_LEN, KL), jnp.float32), -6.0, 6.0)
    return base.astype(jnp.bfloat16)


def with_ends(array, own_key, low, largest):
    index_at = [jax.random.randint(jax.random.fold_in(own_key, axis), (), 0, length) for axis, length in enumerate(array.shape)]
    longest = array.shape.index(max(array.shape))
    neighbour = index_at[:longest] + [(index_at[longest] + 1) % array.shape[longest]] + index_at[longest + 1:]
    return array.at[tuple(index_at)].set(low).at[tuple(neighbour)].set(largest)


def raised(drawn, own_key, source, target, shards_of, factor):
    def block_of(position):
        return (jnp.arange(drawn.shape[position]) // (drawn.shape[position] // shards_of)).reshape((-1,) + (1,) * (drawn.ndim - 1 - position))

    near = jax.random.permutation(own_key, shards_of)[block_of(target)]
    far = (block_of(target) + shards_of // 2) % shards_of
    return jnp.where((block_of(source) == near) | (block_of(source) == far), factor * drawn, drawn)


def block_scale(key, extent, cuts, low, largest):
    factor_of, own = 1.0, jax.random.fold_in(key, 6)
    for dim, shards_of in cuts:
        heights = jnp.exp(jax.random.uniform(jax.random.fold_in(own, dim), (shards_of,), jnp.float32, low / len(cuts), largest / len(cuts)))
        factor_of = factor_of * jnp.repeat(heights, extent[dim] // shards_of).reshape([-1 if axis == dim else 1 for axis in range(len(extent))])
    return factor_of


def routed_block(own_key, own, number, rows, number_of, top, bound, skew):
    order = jax.random.permutation(own_key, number_of)
    crowded, ordinary = shares(number_of, rows * top, bound, skew, True), shares(number_of, rows * top, bound, skew, False)
    places = jnp.arange(number_of)

    def named(sizes, offset_by):
        used = int((sizes > 0).sum())
        fixed = max(1, used // 4)
        moved = fixed + (places - fixed + offset_by * (used - fixed)) % max(1, number_of - fixed)
        return jnp.zeros((number_of,), jnp.int32).at[order[jnp.where(places < fixed, places, moved)]].set(jnp.asarray(sizes, jnp.int32))

    sizes = jnp.where(number % 4 == 0, named(crowded, number // 4), named(ordinary, number - number // 4 - 1))
    mixed = jax.random.permutation(jax.random.fold_in(own, 3), number_of)
    donor, receiver = mixed[0:number_of // 2 * 2:2], mixed[1:number_of // 2 * 2:2]
    slack = jnp.minimum(sizes[donor] - 1, bound - sizes[receiver]) // 2
    slack = jnp.where((donor == order[0]) | (receiver == order[0]) | (sizes[receiver] == 0), 0, jnp.maximum(slack, 0))
    moved = jax.random.randint(jax.random.fold_in(own, 4), (number_of // 2,), 0, 1 << 20) % (slack + 1)
    sizes = sizes.at[donor].add(-moved).at[receiver].add(moved)
    labels = jnp.searchsorted(jnp.cumsum(sizes), jnp.arange(rows * top), side="right").astype(jnp.int32)
    table = labels.reshape(top, rows).T
    table = table[jax.random.permutation(jax.random.fold_in(own, 1), rows)]
    offset_by = jax.random.randint(jax.random.fold_in(own, 2), (rows, 1), 0, top)
    return jnp.take_along_axis(table, (jnp.arange(top)[None, :] + offset_by) % top, axis=1)


def shares(count, total, bound, slope, full):
    portions = [(1 << 20) // math.isqrt(standing ** slope) + 1 for standing in range(1, count + 1)]
    largest = bound if full else min(bound, max(-(-total // count), total * portions[0] // sum(portions)))
    least = 1 if total - largest >= count - 1 else 0
    holding, spare = [largest] + [least] * (count - 1), total - largest - least * (count - 1)
    while spare > 0:
        free = [i for i in range(1, count) if holding[i] < largest] or [i for i in range(1, count) if holding[i] < bound]
        mass, budget = sum([portions[i] for i in free]), spare
        for i in free:
            more = min(bound - holding[i], max(1, budget * portions[i] // mass), spare)
            holding[i] = holding[i] + more
            spare = spare - more
    return np.array(holding)


def bell_draw(rng, dims, deviation, reach, shards=(), kind=jnp.bfloat16):
    level = block_scale(rng, dims, shards, -0.22, 0.18) if shards else 1.0
    array = jax.random.normal(rng, dims, jnp.float32) * deviation * level
    return jnp.minimum(jnp.maximum(array, -reach), reach).astype(kind)


def noise_with(rng, dims, deviation, reach, cuts, heavy, kind=jnp.bfloat16):
    array = deviation * jax.random.normal(rng, dims, jnp.float32)
    if cuts:
        array = array * block_scale(rng, dims, cuts, -0.22, 0.18)
    return jnp.clip(raised(array, jax.random.fold_in(rng, 3), *heavy), -reach, reach).astype(kind)


def setup_inputs(seed: int = 0) -> dict:
    key_list = jax.random.split(jax.random.key(seed), 31)
    tokens = bell_draw(key_list[0], (TOKENS, D), 1.0, 6.0, ((0, 32),))
    lengths = with_ends(jax.random.randint(key_list[1], (TOKENS,), 1, CACHE_LEN + 1), jax.random.fold_in(key_list[1], 1), 1, CACHE_LEN).astype(jnp.int32)
    cache_latent = draw_cache_latent(jax.random.fold_in(key_list[30], 71), 0)
    cache_rope = bell_draw(key_list[3], (TOKENS, ROPE, CACHE_LEN), 1.0, 6.0, ((0, 32),))
    attn_gain = jnp.clip(1.0 + 0.18 * jax.random.normal(key_list[4], (D,), jnp.float32), 0.099609375, 1.8984375).astype(jnp.bfloat16)
    w_dq = bell_draw(key_list[5], (D, QL), D ** -0.5, 0.1875)
    q_gain = jnp.clip(1.0 + 0.18 * jax.random.normal(key_list[6], (QL,), jnp.float32), 0.099609375, 1.8984375).astype(jnp.bfloat16)
    w_q_nope = bell_draw(key_list[7], (QL, HEADS * NOPE), QL ** -0.5, 0.25)
    w_q_rope = bell_draw(key_list[8], (QL, HEADS * ROPE), QL ** -0.5, 0.25)
    w_dkv = bell_draw(key_list[9], (D, KL), D ** -0.5, 0.1875)
    kv_gain = jnp.clip(1.0 + 0.18 * jax.random.normal(key_list[10], (KL,), jnp.float32), 0.099609375, 1.8984375).astype(jnp.bfloat16)
    w_krope = bell_draw(key_list[11], (D, ROPE), D ** -0.5, 0.1875)
    w_uk = bell_draw(key_list[12], (KL, HEADS * NOPE), NOPE ** -0.5, 0.75)
    w_uv = bell_draw(key_list[13], (KL, HEADS * VDIM), KL ** -0.5, 0.375)
    w_o = bell_draw(key_list[14], (HEADS * VDIM, D), (HEADS * VDIM) ** -0.5, 0.1875)
    post_gain = jnp.clip(1.0 + 0.18 * jax.random.normal(key_list[15], (D,), jnp.float32), 0.099609375, 1.8984375).astype(jnp.bfloat16)
    moe_gain = jnp.clip(1.0 + 0.18 * jax.random.normal(key_list[16], (D,), jnp.float32), 0.099609375, 1.8984375).astype(jnp.bfloat16)
    routes_keys = jax.random.split(jax.random.fold_in(key_list[17], 1), TOKENS // SEQ_DEV)
    routes_turns = jax.random.permutation(jax.random.fold_in(key_list[17], 3), TOKENS // SEQ_DEV)
    routes = jax.vmap(lambda own, number: routed_block(jax.random.fold_in(key_list[17], 2), own, number, SEQ_DEV, EXPERTS, TOP_K, CAP, 2))(routes_keys, routes_turns).reshape((TOKENS, TOP_K))
    route_scores = jnp.clip(jnp.exp(math.log(1.0) - 2.9957323 * jax.random.uniform(key_list[18], (TOKENS, TOP_K), jnp.float32) ** block_scale(key_list[18], (TOKENS, TOP_K), ((0, 32),), -0.2, 0.2)), 0.05, 1.0)
    expert_gate = bell_draw(key_list[19], (EXPERTS, D, EFF), D ** -0.5, 0.1875, ((0, 16), (2, 2)))
    expert_up = bell_draw(key_list[20], (EXPERTS, D, EFF), D ** -0.5, 0.1875, ((0, 16), (2, 2)))
    expert_down = bell_draw(key_list[21], (EXPERTS, EFF, D), EFF ** -0.5, 0.25, ((0, 16), (1, 2)))
    shared_gate = bell_draw(key_list[22], (D, SFF), D ** -0.5, 0.1875)
    shared_up = bell_draw(key_list[23], (D, SFF), D ** -0.5, 0.1875)
    shared_down = bell_draw(key_list[24], (SFF, D), SFF ** -0.5, 0.25)
    dense_vec = bell_draw(key_list[25], (D,), D ** -0.5, 0.1875)
    dense_w_gate = bell_draw(key_list[26], (D, DFF), D ** -0.5, 0.1875, ((1, 32),))
    dense_w_up = bell_draw(key_list[27], (D, DFF), D ** -0.5, 0.1875, ((1, 32),))
    dense_w_down = noise_with(key_list[28], (DFF, D), DFF ** -0.5, 0.125, ((0, 32),), (0, 1, 32, 2.75))
    out_gain = jnp.clip(1.0 + 0.18 * jax.random.normal(key_list[29], (D,), jnp.float32), 0.099609375, 1.8984375).astype(jnp.bfloat16)
    return dict(tokens=tokens, lengths=lengths, cache_latent=cache_latent, cache_rope=cache_rope, attn_gain=attn_gain, w_dq=w_dq, q_gain=q_gain, w_q_nope=w_q_nope, w_q_rope=w_q_rope, w_dkv=w_dkv, kv_gain=kv_gain, w_krope=w_krope, w_uk=w_uk, w_uv=w_uv, w_o=w_o, post_gain=post_gain, moe_gain=moe_gain, routes=routes, route_scores=route_scores, expert_gate=expert_gate, expert_up=expert_up, expert_down=expert_down, shared_gate=shared_gate, shared_up=shared_up, shared_down=shared_down, dense_vec=dense_vec, dense_w_gate=dense_w_gate, dense_w_up=dense_w_up, dense_w_down=dense_w_down, out_gain=out_gain)


eps = 1e-06
rope_base = 10000.0
routed_scale = 2.5

def rms_scale(value, gain):
    value = value.astype(jnp.float32)
    inverse = lax.rsqrt(lax.optimization_barrier(jnp.mean(value * value, axis=-1, keepdims=True)) + eps)
    return value * inverse * gain.astype(jnp.float32)

def angles(lengths):
    half = ROPE // 2
    freqs = rope_base ** (-jnp.arange(half, dtype=jnp.float32) / half)
    angle = lengths.astype(jnp.float32)[:, None] * freqs[None, :]
    return (jnp.cos(angle), jnp.sin(angle))

def rotate(value, cosine, sine):
    half = value.shape[-1] // 2
    first, second = (value[..., :half], value[..., half:])
    return jnp.concatenate([first * cosine - second * sine, second * cosine + first * sine], axis=-1)

def slot_table(ids, scores, experts, cap):
    rows, top = ids.shape
    norm = scores / lax.optimization_barrier(jnp.sum(scores, axis=1, keepdims=True)) * routed_scale
    flat = ids.reshape(-1)
    onehot = (flat[:, None] == jnp.arange(experts, dtype=jnp.int32)[None, :]).astype(jnp.int32)
    rank = jnp.cumsum(onehot, axis=0) - 1
    hit = onehot[:, :, None] * (rank[:, :, None] == jnp.arange(cap, dtype=jnp.int32)[None, None, :]).astype(jnp.int32)
    owner = jnp.arange(rows * top, dtype=jnp.int32) // top
    token_of = lax.optimization_barrier(jnp.sum(hit * owner[:, None, None], axis=0)).astype(jnp.int32)
    weight_of = lax.optimization_barrier(jnp.sum(hit.astype(norm.dtype) * norm.reshape(-1)[:, None, None], axis=0))
    return (token_of, weight_of)

def attend_block(block, weights):
    tokens, lengths, latent, rope_keys = block
    attn_gain, w_dq, q_gain, w_q_nope, w_q_rope, w_dkv, kv_gain, w_krope, w_uk, w_uv, w_o, post_gain = weights
    f32 = jnp.float32
    bf16 = jnp.bfloat16
    seqs = tokens.shape[0]
    normed = rms_scale(tokens, attn_gain).astype(bf16)
    q_normed = rms_scale(jnp.dot(normed, w_dq, preferred_element_type=f32), q_gain).astype(bf16)
    q_nope = jnp.dot(q_normed, w_q_nope, preferred_element_type=f32).astype(bf16).reshape(seqs, HEADS, NOPE)
    cosine, sine = angles(lengths)
    q_raw = jnp.dot(q_normed, w_q_rope, preferred_element_type=f32).reshape(seqs, HEADS, ROPE)
    q_rot = rotate(q_raw, cosine[:, None, :], sine[:, None, :]).astype(bf16)
    new_latent = rms_scale(jnp.dot(normed, w_dkv, preferred_element_type=f32), kv_gain).astype(bf16)
    new_rope = rotate(jnp.dot(normed, w_krope, preferred_element_type=f32), cosine, sine).astype(bf16)
    query_lat = jnp.einsum('shn,chn->shc', q_nope.astype(f32), w_uk.reshape(KL, HEADS, NOPE).astype(f32)).astype(bf16)
    scale = (NOPE + ROPE) ** (-0.5)
    past = jnp.einsum('shc,slc->shl', query_lat.astype(f32), latent.astype(f32))
    past = (past + jnp.einsum('shr,srl->shl', q_rot.astype(f32), rope_keys.astype(f32))) * scale
    own = jnp.einsum('shc,sc->sh', query_lat.astype(f32), new_latent.astype(f32))
    own = (own + jnp.einsum('shr,sr->sh', q_rot.astype(f32), new_rope.astype(f32))) * scale
    valid = jnp.arange(CACHE_LEN, dtype=jnp.int32)[None, None, :] < lengths[:, None, None]
    top = jnp.maximum(lax.optimization_barrier(jnp.max(jnp.where(valid, past, -1e+30), axis=-1)), own)
    past_weight = jnp.where(valid, jnp.exp(past - top[..., None]), 0.0)
    own_weight = jnp.exp(own - top)
    total = lax.optimization_barrier(jnp.sum(past_weight, axis=-1)) + own_weight
    past_prob = (past_weight / total[..., None]).astype(bf16)
    own_prob = (own_weight / total).astype(bf16)
    mixed = jnp.einsum('shl,slc->shc', past_prob.astype(f32), latent.astype(f32))
    mixed = (mixed + own_prob.astype(f32)[..., None] * new_latent.astype(f32)[:, None, :]).astype(bf16)
    head_out = jnp.einsum('shc,chv->shv', mixed.astype(f32), w_uv.reshape(KL, HEADS, VDIM).astype(f32)).astype(bf16)
    attn_out = jnp.dot(head_out.reshape(seqs, HEADS * VDIM), w_o, preferred_element_type=f32)
    first = (tokens.astype(f32) + rms_scale(attn_out, post_gain)).astype(bf16)
    return (first, new_latent)

def reference(tokens, lengths, cache_latent, cache_rope, attn_gain, w_dq, q_gain, w_q_nope, w_q_rope, w_dkv, kv_gain, w_krope, w_uk, w_uv, w_o, post_gain, moe_gain, routes, route_scores, expert_gate, expert_up, expert_down, shared_gate, shared_up, shared_down, dense_vec, dense_w_gate, dense_w_up, dense_w_down, out_gain):
    f32 = jnp.float32
    bf16 = jnp.bfloat16
    groups = TOKENS // SEQ_DEV
    weights = (attn_gain, w_dq, q_gain, w_q_nope, w_q_rope, w_dkv, kv_gain, w_krope, w_uk, w_uv, w_o, post_gain)
    blocks = (tokens.reshape(groups, SEQ_DEV, D), lengths.reshape(groups, SEQ_DEV), cache_latent.reshape(groups, SEQ_DEV, CACHE_LEN, KL), cache_rope.reshape(groups, SEQ_DEV, ROPE, CACHE_LEN))
    first, new_latent = lax.map(partial(attend_block, weights=weights), blocks)
    first = first.reshape(TOKENS, D)
    new_latent = new_latent.reshape(TOKENS, KL)
    moe_in = rms_scale(first, moe_gain).astype(bf16)
    shared_act = (jax.nn.silu(jnp.dot(moe_in, shared_gate, preferred_element_type=f32)) * jnp.dot(moe_in, shared_up, preferred_element_type=f32)).astype(bf16)
    shared_out = jnp.dot(shared_act, shared_down, preferred_element_type=f32)
    dense_act = (jax.nn.silu(jnp.dot(moe_in, dense_w_gate, preferred_element_type=f32)) * jnp.dot(moe_in, dense_w_up, preferred_element_type=f32)).astype(bf16)
    dense_out = jnp.dot(dense_act, dense_w_down, preferred_element_type=f32)
    gate = jax.nn.sigmoid(jnp.dot(moe_in, dense_vec, preferred_element_type=f32))
    token_all, weight_all = jax.vmap(partial(slot_table, experts=EXPERTS, cap=CAP))(routes.reshape(groups, SEQ_DEV, TOP_K), route_scores.reshape(groups, SEQ_DEV, TOP_K))
    base = (jnp.arange(groups, dtype=jnp.int32) * SEQ_DEV)[:, None]

    def expert_step(routed, expert):
        where_rows = (lax.dynamic_index_in_dim(token_all, expert, 1, keepdims=False) + base).reshape(-1).astype(jnp.int32)
        weight = lax.dynamic_index_in_dim(weight_all, expert, 1, keepdims=False).reshape(-1)
        rows = moe_in[where_rows]
        hidden_gate = jnp.dot(rows, expert_gate[expert], preferred_element_type=f32)
        hidden_up = jnp.dot(rows, expert_up[expert], preferred_element_type=f32)
        act = (jax.nn.silu(hidden_gate) * hidden_up).astype(bf16)
        act_parts = act.astype(f32).reshape(-1, N_TP, EFF // N_TP)
        down_parts = expert_down[expert].astype(f32).reshape(N_TP, EFF // N_TP, D)
        parts = jnp.einsum('rtf,tfd->rtd', act_parts, down_parts).astype(bf16).astype(f32)
        out = lax.optimization_barrier(jnp.sum(parts, axis=1))
        return (routed.at[where_rows].add(out * weight[:, None].astype(f32)), None)
    routed, _ = lax.scan(expert_step, jnp.zeros((TOKENS, D), f32), jnp.arange(EXPERTS, dtype=jnp.int32))
    mixture = routed + shared_out + gate[:, None] * dense_out
    hidden_out = (first.astype(f32) + rms_scale(mixture, out_gain)).astype(bf16)
    return (hidden_out, new_latent)
```

```python
import functools

import jax
import jax.numpy as jnp
from jax import lax
from jax.experimental import pallas as pl
from jax.experimental.pallas import tpu as pltpu
from jax.sharding import PartitionSpec as P

HEADS = 16
NOPE = 64
ROPE = 32
VDIM = 64


eps = 1e-06
rope_base = 10000.0
routed_scale = 2.5


def rms_scale(value, gain):
    value = value.astype(jnp.float32)
    inverse = lax.rsqrt(jnp.mean(value * value, axis=-1, keepdims=True) + eps)
    return value * inverse * gain.astype(jnp.float32)


def angles(lengths, rope_dim):
    half = rope_dim // 2
    freqs = rope_base ** (-jnp.arange(half, dtype=jnp.float32) / half)
    angle = lengths.astype(jnp.float32)[:, None] * freqs[None, :]
    return (jnp.cos(angle), jnp.sin(angle))


def attention_kernel(
    batch,
    experts,
    lens_ref,
    tokens_ref,
    cos_ref,
    sin_ref,
    meta_ref,
    attn_gain,
    q_gain,
    kv_gain,
    post_gain,
    moe_gain,
    dense_vec,
    *refs,
):
    f32, bf16 = jnp.float32, jnp.bfloat16
    hbm, (first_ref, x_ref, latent_out), bufs = refs[:10], refs[10:13], refs[13:23]
    query, spun, mixed, sem, cache_sem = refs[23:]
    w_dq, w_dkv, w_krope, w_q_nope, w_q_rope, w_uk, latent, rope, w_uv, w_o = bufs
    seqs, length, wide = latent.shape
    width = tokens_ref.shape[1]

    weights = [0, 1, 2, 3, 4, 5, 8, 9]
    loads = {i: pltpu.make_async_copy(hbm[i], bufs[i], sem.at[i]) for i in weights}

    def cache_load(s):
        return (
            pltpu.make_async_copy(hbm[6].at[s], latent.at[s], cache_sem.at[0, s]),
            pltpu.make_async_copy(hbm[7].at[s], rope.at[s], cache_sem.at[1, s]),
        )

    for i in weights[:6]:
        loads[i].start()

    @pl.loop(0, seqs)
    def _(s):
        for load in cache_load(s):
            load.start()

    for i in weights[6:]:
        loads[i].start()

    def mul(a, b):
        return jnp.dot(a, b, preferred_element_type=f32)

    def mul_t(a, b):
        return lax.dot_general(a, b, (((1,), (1,)), ((), ())), preferred_element_type=f32)

    tokens = tokens_ref[...].astype(f32)
    normed = rms_scale(tokens, attn_gain[...]).astype(bf16)
    loads[0].wait()
    q_normed = rms_scale(mul(normed, w_dq[...]), q_gain[...]).astype(bf16)
    loads[1].wait()
    new_latent = rms_scale(mul(normed, w_dkv[...]), kv_gain[...]).astype(bf16)
    latent_out[...] = new_latent
    fresh = new_latent.astype(f32)
    loads[2].wait()
    half = ROPE // 2
    raw = mul(normed, w_krope[...])
    swapped = jnp.concatenate([raw[:, half:], raw[:, :half]], axis=1)
    new_rope = (raw * cos_ref[:, :ROPE] + swapped * sin_ref[:, :ROPE]).astype(bf16).astype(f32)
    loads[3].wait()
    q_nope = mul(q_normed, w_q_nope[...]).astype(bf16)
    loads[4].wait()
    raw = mul(q_normed, w_q_rope[...])
    span = raw.shape[1]
    lane = lax.broadcasted_iota(jnp.int32, raw.shape, 1)
    swapped = jnp.where(
        lane % ROPE < half, pltpu.roll(raw, span - half, 1), pltpu.roll(raw, half, 1)
    )
    q_rot = (raw * cos_ref[...] + swapped * sin_ref[...]).astype(bf16).astype(f32)
    for h in range(HEADS):
        spun[:, h, :] = q_rot[:, h * ROPE : (h + 1) * ROPE]
    loads[5].wait()
    low = lax.broadcasted_iota(jnp.int32, (seqs, 2 * NOPE), 1) < NOPE
    for pair in range(HEADS // 2):
        at = slice(pair * 2 * NOPE, (pair + 1) * 2 * NOPE)
        both = q_nope[:, at].astype(f32)
        both = jnp.concatenate([jnp.where(low, both, 0.0), jnp.where(low, 0.0, both)], axis=0)
        lat = mul_t(both.astype(bf16), w_uk[:, at]).astype(bf16).astype(f32)
        query[:, 2 * pair, :] = lat[:seqs]
        query[:, 2 * pair + 1, :] = lat[seqs:]

    scale = (NOPE + ROPE) ** (-0.5)
    place = lax.broadcasted_iota(jnp.int32, (HEADS, length), 1)
    row = lax.broadcasted_iota(jnp.int32, (seqs, 1), 0)

    @pl.loop(0, seqs // batch)
    def _(step):
        ids = [step * batch + i for i in range(batch)]
        for s in ids:
            for load in cache_load(s):
                load.wait()
        for s in ids:
            mine, turned, keys = query[s], spun[s], latent[s]
            own_key = jnp.sum(jnp.where(row == s, fresh, 0.0), axis=0, keepdims=True)
            own_rope = jnp.sum(jnp.where(row == s, new_rope, 0.0), axis=0, keepdims=True)
            past = (mul_t(mine.astype(bf16), keys) + mul(turned.astype(bf16), rope[s])) * scale
            own = jnp.sum(mine * own_key, axis=1, keepdims=True)
            own = (own + jnp.sum(turned * own_rope, axis=1, keepdims=True)) * scale
            valid = place < lens_ref[s]
            top = jnp.max(jnp.where(valid, past, -1e30), axis=1, keepdims=True)
            top = jnp.maximum(top, own)
            past = jnp.where(valid, jnp.exp(past - top), 0.0)
            own = jnp.exp(own - top)
            total = jnp.sum(past, axis=1, keepdims=True) + own
            out = mul((past / total).astype(bf16), keys)
            mixed[s] = out + (own / total).astype(bf16).astype(f32) * own_key

    loads[8].wait()
    parts = []
    for pair in range(HEADS // 2):
        at = slice(pair * 2 * VDIM, (pair + 1) * 2 * VDIM)
        both = jnp.concatenate([mixed[:, 2 * pair, :], mixed[:, 2 * pair + 1, :]], axis=0)
        both = mul(both.astype(bf16), w_uv[:, at])
        lane = lax.broadcasted_iota(jnp.int32, (seqs, 2 * VDIM), 1)
        parts.append(jnp.where(lane < VDIM, both[:seqs], both[seqs:]))
    head_out = jnp.concatenate(parts, axis=1).astype(bf16)
    loads[9].wait()
    first = (tokens + rms_scale(mul(head_out, w_o[...]), post_gain[...])).astype(bf16)
    first_ref[...] = first
    moe_in = rms_scale(first, moe_gain[...]).astype(bf16)
    x_ref[:, :width] = moe_in
    gate = jnp.sum(moe_in.astype(f32) * dense_vec[...].astype(f32), axis=1, keepdims=True)
    gate = jax.nn.sigmoid(gate)
    lane = lax.broadcasted_iota(jnp.int32, meta_ref.shape, 1)
    columns = experts + 1
    rest = jnp.where(lane % columns == experts, gate, meta_ref[...])
    out = jnp.zeros_like(rest)
    for part in range(PARTS):
        piece = rest.astype(bf16).astype(f32)
        here = (lane >= part * columns) & (lane < (part + 1) * columns)
        out = jnp.where(here, piece, out)
        rest = rest - piece
    x_ref[:, width:] = out.astype(bf16)


def attention(tokens, lengths, meta, experts, gains, big):
    f32, bf16 = jnp.float32, jnp.bfloat16
    seqs, width = tokens.shape
    cosine, sine = angles(lengths, ROPE)
    cosine = jnp.tile(jnp.concatenate([cosine, cosine], axis=1), (1, HEADS))
    sine = jnp.tile(jnp.concatenate([-sine, sine], axis=1), (1, HEADS))
    wide = big[6].shape[2]
    batch = 4 if seqs % 4 == 0 else 1
    vmem = pl.BlockSpec(memory_space=pltpu.VMEM)
    return pl.pallas_call(
        functools.partial(attention_kernel, batch, experts),
        out_shape=(
            jax.ShapeDtypeStruct((seqs, width), bf16),
            jax.ShapeDtypeStruct((seqs, width + meta.shape[1]), bf16),
            jax.ShapeDtypeStruct((seqs, wide), bf16),
        ),
        in_specs=[pl.BlockSpec(memory_space=pltpu.SMEM)]
        + [vmem] * 10
        + [pl.BlockSpec(memory_space=pltpu.HBM)] * 10,
        out_specs=(vmem, vmem, vmem),
        scratch_shapes=[pltpu.VMEM(w.shape, w.dtype) for w in big]
        + [
            pltpu.VMEM((seqs, HEADS, wide), f32),
            pltpu.VMEM((seqs, HEADS, ROPE), f32),
            pltpu.VMEM((seqs, HEADS, wide), f32),
            pltpu.SemaphoreType.DMA((10,)),
            pltpu.SemaphoreType.DMA((2, seqs)),
        ],

        name="attention",
    )(lengths, tokens, cosine, sine, meta, *[g.reshape(1, -1) for g in gains], *big)


MESH = pl.DeviceIdType.MESH
PARTS = 3


def partner(me, k, count):
    other, bit = me, 1
    while bit < count:
        other = other + bit * ((k // bit) % 2) * (1 - 2 * ((me // bit) % 2))
        bit *= 2
    return other


def meta_width(experts):
    return -(-PARTS * (experts + 1) // 128) * 128


def exchange_kernel(
    count,
    groups,
    x_ref,
    first_ref,
    gain_ref,
    eg_hbm,
    eu_hbm,
    ed_hbm,
    dg_hbm,
    du_hbm,
    dd_hbm,
    sg_hbm,
    su_hbm,
    sd_hbm,
    out_ref,
    eg,
    eu,
    ed,
    dg,
    du,
    dd,
    sg,
    su,
    sd,
    rows,
    keep,
    to_sib,
    from_sib,
    to_home,
    from_home,
    load_sem,
    row_send,
    row_recv,
    relay_send,
    relay_recv,
    sib_send,
    sib_recv,
    home_send,
    home_recv,
):
    f32, bf16 = jnp.float32, jnp.bfloat16
    seqs, wide = x_ref.shape
    width = first_ref.shape[1]
    me = lax.axis_index("ep")
    core = lax.axis_index("tp")
    sibling = (me, 1 - core)
    size = count // groups

    loads = [
        pltpu.make_async_copy(src, dst, load_sem.at[i])
        for i, (src, dst) in enumerate(
            (
                (sg_hbm, sg),
                (su_hbm, su),
                (sd_hbm, sd),
                (eg_hbm.at[0], eg),
                (eu_hbm.at[0], eu),
                (dg_hbm, dg),
                (du_hbm, du),
                (ed_hbm.at[0], ed),
                (dd_hbm, dd),
            )
        )
    ]
    for load in loads:
        load.start()

    barrier = pltpu.get_barrier_semaphore()
    pl.semaphore_signal(barrier, inc=1, device_id=sibling, device_id_type=MESH)

    @pl.loop(1, count)
    def _(k):
        pl.semaphore_signal(
            barrier, inc=1, device_id=(partner(me, k, count), core), device_id_type=MESH
        )

    pl.semaphore_wait(barrier, count)

    def row_copy(k, src, hop):
        return pltpu.make_async_remote_copy(
            src_ref=src,
            dst_ref=rows.at[0, k],
            send_sem=row_send.at[k],
            recv_sem=row_recv.at[k],
            device_id=(partner(me, hop, count), core),
            device_id_type=MESH,
        )

    def relay_copy(k, src):
        return pltpu.make_async_remote_copy(
            src_ref=src,
            dst_ref=rows.at[1, k],
            send_sem=relay_send.at[k],
            recv_sem=relay_recv.at[k],
            device_id=sibling,
            device_id_type=MESH,
        )

    def sib_copy(g):
        return pltpu.make_async_remote_copy(
            src_ref=to_sib.at[pl.ds(g * size, size)],
            dst_ref=from_sib.at[pl.ds(g * size, size)],
            send_sem=sib_send.at[g],
            recv_sem=sib_recv.at[g],
            device_id=sibling,
            device_id_type=MESH,
        )

    def home_copy(k, hop):
        return pltpu.make_async_remote_copy(
            src_ref=to_home.at[k],
            dst_ref=from_home.at[k],
            send_sem=home_send.at[k],
            recv_sem=home_recv.at[k],
            device_id=(partner(me, hop, count), core),
            device_id_type=MESH,
        )

    for g in range(1, groups):
        row_copy(g * size, x_ref, g * size).start()

    @pl.loop(1, size)
    def _(m):
        row_copy(m, x_ref, m).start()

    relay_copy(0, x_ref).start()
    own = pltpu.make_async_copy(x_ref, rows.at[0, 0], row_recv.at[0])
    own.start()

    for load in loads[:3]:
        load.wait()
    mine = x_ref[:, :width]
    hidden = (
        jax.nn.silu(jnp.dot(mine, sg[...], preferred_element_type=f32))
        * jnp.dot(mine, su[...], preferred_element_type=f32)
    ).astype(bf16)
    total = jnp.dot(hidden, sd[...], preferred_element_type=f32)
    for g in range(1, groups):
        row_copy(g * size, x_ref, g * size).wait_recv()

        @pl.loop(1, size)
        def _(m):
            row_copy(g * size + m, rows.at[0, g * size], m).start()

    for load in loads[3:]:
        load.wait()
    own.wait()

    lane = lax.broadcasted_iota(jnp.int32, (1, wide - width), 1)
    columns = count + 1

    def picked(meta, column):
        chosen = lane == column
        for part in range(1, PARTS):
            chosen = chosen | (lane == column + part * columns)
        return jnp.sum(jnp.where(chosen, meta, 0.0), axis=1, keepdims=True)

    def send_home(g):
        sib_copy(g).wait_recv()
        part = keep[g * size : (g + 1) * size] + from_sib[g * size : (g + 1) * size].astype(f32)
        to_home[g * size : (g + 1) * size] = part.astype(bf16)

        keep[g * size] = part[0]

        @pl.loop(1, size)
        def _(m):
            home_copy(g * size + m, m).start()

    def plane_sum(g):
        @pl.loop(1, size)
        def _(m):
            home_copy(g * size + m, m).wait_recv()

        part = keep[g * size]
        for m in range(1, size):
            part = part + from_home[g * size + m].astype(f32)
        return part

    def send_far(g):
        to_home[g * size] = plane_sum(g).astype(bf16)
        home_copy(g * size, g * size).start()

    order = list(range(1, groups)) + [0]
    for turn, g in enumerate(order):
        if g > 0:
            relay_copy(g * size, rows.at[0, g * size]).start()

        @pl.loop(g * size + 1, (g + 1) * size)
        def _(k):
            row_copy(k, x_ref, 1).wait_recv()
            relay_copy(k, rows.at[0, k]).start()

        if turn > 0:
            send_home(order[turn - 1])

        @pl.loop(g * size, (g + 1) * size)
        def _(k):
            relay_copy(k, x_ref).wait_recv()

        block = rows[:, g * size : (g + 1) * size].reshape(2 * size * seqs, wide)
        values, meta = block[:, :width], block[:, width:].astype(f32)
        act = (
            jax.nn.silu(jnp.dot(values, eg[...], preferred_element_type=f32))
            * jnp.dot(values, eu[...], preferred_element_type=f32)
        ).astype(bf16)
        routed = jnp.dot(act, ed[...], preferred_element_type=f32).astype(bf16).astype(f32)
        act = (
            jax.nn.silu(jnp.dot(values, dg[...], preferred_element_type=f32))
            * jnp.dot(values, du[...], preferred_element_type=f32)
        ).astype(bf16)
        dense = jnp.dot(act, dd[...], preferred_element_type=f32)
        part = routed * picked(meta, me) + dense * picked(meta, count)
        part = part.reshape(2, size, seqs, width)
        to_sib[g * size : (g + 1) * size] = part[1].astype(bf16)
        sib_copy(g).start()
        keep[g * size : (g + 1) * size] = part[0]

    send_home(order[-1])
    for g in range(1, groups):
        send_far(g)
    total = total + plane_sum(0)
    for g in range(1, groups):
        home_copy(g * size, g * size).wait_recv()
        total = total + from_home[g * size].astype(f32)
    inverse = lax.rsqrt(jnp.mean(total * total, axis=-1, keepdims=True) + eps)
    out_ref[...] = (
        first_ref[...].astype(f32) + total * inverse * gain_ref[...].astype(f32)
    ).astype(bf16)

    relay_copy(0, x_ref).wait_send()

    @pl.loop(1, count)
    def _(k):
        row_copy(k, x_ref, 1).wait_send()
        relay_copy(k, rows.at[0, k]).wait_send()
        home_copy(k, 1).wait_send()

    for g in range(groups):
        sib_copy(g).wait_send()


def exchange(rows, first, gain, expert, dense, shared):
    bf16, f32 = jnp.bfloat16, jnp.float32
    count = lax.axis_size("ep")
    groups = min(4, count)
    seqs, width = first.shape
    wide = rows.shape[1]
    any_space = pl.BlockSpec(memory_space=pltpu.HBM)
    vmem = pl.BlockSpec(memory_space=pltpu.VMEM)
    dma = pltpu.SemaphoreType.DMA
    weights = list(expert) + list(dense) + list(shared)
    return pl.pallas_call(
        functools.partial(exchange_kernel, count, groups),
        out_shape=jax.ShapeDtypeStruct((seqs, width), bf16),
        in_specs=[vmem] * 3 + [any_space] * 9,
        out_specs=vmem,
        scratch_shapes=[pltpu.VMEM(w.shape[-2:], w.dtype) for w in weights]
        + [
            pltpu.VMEM((2, count, seqs, wide), bf16),
            pltpu.VMEM((count, seqs, width), f32),
            pltpu.VMEM((count, seqs, width), bf16),
            pltpu.VMEM((count, seqs, width), bf16),
            pltpu.VMEM((count, seqs, width), bf16),
            pltpu.VMEM((count, seqs, width), bf16),
            dma((9,)),
            dma((count,)),
            dma((count,)),
            dma((count,)),
            dma((count,)),
            dma((groups,)),
            dma((groups,)),
            dma((count,)),
            dma((count,)),
        ],
        compiler_params=pltpu.CompilerParams(
            collective_id=0, has_side_effects=True
        ),
        name="exchange",
    )(rows, first, gain.reshape(1, width), *weights)


def meta_columns(routes, scores, experts):
    norm = scores / jnp.sum(scores, axis=1, keepdims=True) * routed_scale
    lane = jnp.arange(meta_width(experts), dtype=jnp.int32) % (experts + 1)
    named = routes[:, :, None] == lane[None, None, :]
    return jnp.sum(jnp.where(named, norm[:, :, None], 0.0), axis=1)


def shards(
    tokens,
    lengths,
    cache_latent,
    cache_rope,
    attn_gain,
    w_dq,
    q_gain,
    w_q_nope,
    w_q_rope,
    w_dkv,
    kv_gain,
    w_krope,
    w_uk,
    w_uv,
    w_o,
    post_gain,
    moe_gain,
    routes,
    route_scores,
    expert_gate,
    expert_up,
    expert_down,
    shared_gate,
    shared_up,
    shared_down,
    dense_vec,
    dense_w_gate,
    dense_w_up,
    dense_w_down,
    out_gain,
):
    experts = expert_gate.shape[0] * lax.axis_size("ep")
    first, rows, new_latent = attention(
        tokens,
        lengths,
        meta_columns(routes, route_scores, experts),
        experts,
        (attn_gain, q_gain, kv_gain, post_gain, moe_gain, dense_vec),
        (w_dq, w_dkv, w_krope, w_q_nope, w_q_rope, w_uk, cache_latent, cache_rope, w_uv, w_o),
    )
    hidden_out = exchange(
        rows,
        first,
        out_gain,
        (expert_gate, expert_up, expert_down),
        (dense_w_gate, dense_w_up, dense_w_down),
        (shared_gate, shared_up, shared_down),
    )
    return (hidden_out, new_latent)


def solution(mesh):
    return jax.shard_map(
        shards,
        mesh=mesh,
        in_specs=(
            P(("ep", "tp"), None),
            P(("ep", "tp")),
            P(("ep", "tp"), None, None),
            P(("ep", "tp"), None, None),
            P(),
            P(),
            P(),
            P(),
            P(),
            P(),
            P(),
            P(),
            P(),
            P(),
            P(),
            P(),
            P(),
            P(("ep", "tp"), None),
            P(("ep", "tp"), None),
            P("ep", None, "tp"),
            P("ep", None, "tp"),
            P("ep", "tp", None),
            P(),
            P(),
            P(),
            P(),
            P(None, ("ep", "tp")),
            P(None, ("ep", "tp")),
            P(("ep", "tp"), None),
            P(),
        ),
        out_specs=(P(("ep", "tp"), None), P(("ep", "tp"), None)),
        check_vma=False,
    )
```
